128 devices in a mesh: ep: 128 (over z, y, x, core).
Axes of the slice: x: 4, y: 4, z: 4, core: 2. Of those that a mesh axis runs over, the one named last changes fastest.
Arguments:
- tokens: bfloat16 [2304, 2048], P('ep'), may hold values from -6 to 6
- attn_norm_gain: float32 [2048], replicated, may hold values from 0.1 to 1.9
- w_query: bfloat16 [2048, 512], replicated, may hold values from -0.125 to 0.125
- w_key: bfloat16 [2048, 128], replicated, may hold values from -0.125 to 0.125
- w_value: bfloat16 [2048, 128], replicated, may hold values from -0.125 to 0.125
- w_forget: bfloat16 [2048, 8], replicated, may hold values from -0.125 to 0.125
- forget_bias: float32 [8], replicated, may hold values from 0.5 to 4
- w_attn_out: bfloat16 [512, 2048], replicated, may hold values from -0.25 to 0.25
- cache_keys: bfloat16 [2304, 1024, 128], P('ep'), may hold values from -72 to 72
- cache_values: bfloat16 [2304, 1024, 128], P('ep'), may hold values from -6 to 6
- cache_logcum: float32 [2304, 8, 1024], P('ep'), as said below
- cache_lengths: int32 [2304], P('ep'), may hold values from 128 to 1024
- expert_norm_gain: float32 [2048], replicated, may hold values from 0.4 to 40
- expert_ids: int32 [2304, 6], P('ep'), may hold values from 0 to 127, all different within a row; in each aligned block of 18 rows (0 to 17, 18 to 35, ...) at most 2 rows name the same one
- expert_weights: float32 [2304, 6], P('ep'), may hold values from 0.1 to 1
- w_expert_gate: bfloat16 [128, 2048, 512], P('ep'), may hold values from -0.125 to 0.125
- w_expert_up: bfloat16 [128, 2048, 512], P('ep'), may hold values from -0.125 to 0.125
- w_expert_down: bfloat16 [128, 512, 2048], P('ep'), may hold values from -0.25 to 0.25
- w_dense_gate: bfloat16 [2048, 4096], P(None, 'ep'), may hold values from -0.125 to 0.125
- w_dense_up: bfloat16 [2048, 4096], P(None, 'ep'), may hold values from -2 to 2
- w_dense_down: bfloat16 [4096, 2048], P('ep'), may hold values from -0.09375 to 0.09375
- dense_norm_gain: float32 [4096], replicated, may hold values from 0.1 to 1.9
- branch_gate: float32 [2048], replicated, may hold values from -0.125 to 0.125
Outputs:
- result: bfloat16 [2304, 2048], P('ep')
The draws below stay inside these ranges and needn't reach their ends.
Inputs may be any that keep to these rules, and one draw needn't show every extreme that they name: `cache_logcum`: along the positions of each sequence and head the values never rise. `expert_ids`: each row names 6 different experts; among the rows of one device no expert is named by more than 2 rows, and in every draw some device names some expert exactly 2 times.
All inputs are finite; a program needn't handle non-finite values.
Results may differ from the reference program's by a relative error of at most 0.012.
The reference program's roundings to bfloat16 on the way count: a program that leaves them out, or rounds other values in their place, can miss the bound.
Values may be sent and summed in bfloat16 or wider, within the bound.
A program may use at most 128 MiB of HBM per device.

```python
import math
import jax
import jax.numpy as jnp
import numpy as np
from jax import lax

D = 2048
HEADS = 8
KV_HEADS = 2
HEAD_DIM = 64
EXPERT_FF = 512
DENSE_FF = 4096
TOPK = 6
SEQ_DEV = 18
CACHE_POSITIONS = 1024
SEQS = 2304
EXPERTS = 128
CAP = 2
N_EP = 128


def draw_cache_keys(key, part):
    tensor_extent = (SEQS, CACHE_POSITIONS, KV_HEADS * HEAD_DIM)
    base = jnp.clip(jax.random.normal(jax.random.fold_in(key, 11), tensor_extent, jnp.float32), -6.0, 6.0)
    values = base
    return jnp.clip(values, -72.0, 72.0).astype(jnp.bfloat16)


def draw_cache_logcum(key, part):
    tensor_extent = (SEQS, HEADS, CACHE_POSITIONS)
    order = jax.random.permutation(jax.random.fold_in(key, 21), HEADS)
    gradual_decay = (order < HEADS // 2)[None, :, None]
    chain_total = jax.random.uniform(jax.random.fold_in(key, 22), (SEQS, HEADS, 1), jnp.float32, 0.3, 1.5)
    fast_span = jax.random.uniform(jax.random.fold_in(key, 23), (SEQS, HEADS, 1), jnp.float32, 30.0, 100.0)
    decay_speed = jnp.where(gradual_decay, chain_total / CACHE_POSITIONS, 1.0 / fast_span)
    sequence_multiplier = jnp.exp(jax.random.uniform(jax.random.fold_in(key, 24), (SEQS, 1, 1), jnp.float32, -0.7, 0.7))
    coarse_estimate = jnp.exp(jax.random.uniform(jax.random.fold_in(key, 25), tensor_extent, jnp.float32, -0.7, 0.7))
    spike_position = jax.random.uniform(jax.random.fold_in(key, 26), tensor_extent, jnp.float32) < 3.0 / CACHE_POSITIONS
    spike_amount = -jnp.log(jax.random.uniform(jax.random.fold_in(key, 27), tensor_extent, jnp.float32, 0.5, 0.8))
    step_numbers = decay_speed * sequence_multiplier * coarse_estimate + jnp.where(spike_position & gradual_decay, spike_amount, 0.0)
    return -jnp.cumsum(step_numbers, axis=2)


def draw_expert_norm_gain(key, part):
    base = 1.0 + 0.18 * jnp.clip(jax.random.normal(jax.random.fold_in(key, 31), (D,), jnp.float32), -3.0, 3.0)
    return base


def draw_w_dense_up(key, part):
    normal_part = jnp.clip(jax.random.normal(jax.random.fold_in(key, 41), (D, DENSE_FF), jnp.float32), -6.0, 6.0)
    column = jnp.arange(DENSE_FF, dtype=jnp.float32)[None, :] / DENSE_FF
    scale = 3.0 ** column * jnp.exp(jax.random.uniform(jax.random.fold_in(key, 43), (1, DENSE_FF), jnp.float32, -0.3, 0.3))
    return jnp.clip(normal_part * D ** (-0.5) * scale, -2.0, 2.0).astype(jnp.bfloat16)


def with_ends(drawn, key, smallest, largest):
    shape = drawn.shape
    spot = [jax.random.randint(jax.random.fold_in(key, axis), (), 0, shape[axis]) for axis in range(len(shape))]
    drawn = drawn.at[tuple(spot)].set(smallest)
    longest = shape.index(max(shape))
    spot[longest] = (spot[longest] + 1) % shape[longest]
    return drawn.at[tuple(spot)].set(largest)


def steps_of(key, extent, cuts, least, top_value):
    factor_of = 1.0
    for axis_at, parts in cuts:
        steps = jax.random.uniform(jax.random.fold_in(jax.random.fold_in(key, 6), axis_at), (parts,), jnp.float32, least / len(cuts), top_value / len(cuts))
        factor_of = factor_of * jnp.repeat(jnp.exp(steps), extent[axis_at] // parts).reshape((-1,) + (1,) * (len(extent) - 1 - axis_at))
    return factor_of


def deal_out(rng, own, number, rows, number_of, top, most, lean):
    sequence = jax.random.permutation(rng, number_of)
    crowded, usual = shares(number_of, rows * top, most, lean, True), shares(number_of, rows * top, most, lean, False)
    places = jnp.arange(number_of)

    def named(tallies, rotation):
        used = int((tallies > 0).sum())
        fixed = max(1, used // 4)
        shifted = fixed + (places - fixed + rotation * (used - fixed)) % max(1, number_of - fixed)
        return jnp.zeros((number_of,), jnp.int32).at[sequence[jnp.where(places < fixed, places, shifted)]].set(jnp.asarray(tallies, jnp.int32))

    tallies = jnp.where(number % 4 == 0, named(crowded, number // 4), named(usual, number - number // 4 - 1))
    mixed = jax.random.permutation(jax.random.fold_in(own, 3), number_of)
    giver, receiver = mixed[0:number_of // 2 * 2:2], mixed[1:number_of // 2 * 2:2]
    margin = jnp.minimum(tallies[giver] - 1, most - tallies[receiver]) // 2
    margin = jnp.where((giver == sequence[0]) | (receiver == sequence[0]) | (tallies[receiver] == 0), 0, jnp.maximum(margin, 0))
    shifted = jax.random.randint(jax.random.fold_in(own, 4), (number_of // 2,), 0, 1 << 20) % (margin + 1)
    tallies = tallies.at[giver].add(-shifted).at[receiver].add(shifted)
    labels = jnp.searchsorted(jnp.cumsum(tallies), jnp.arange(rows * top), side="right").astype(jnp.int32)
    listing = labels.reshape(top, rows).T
    listing = listing[jax.random.permutation(jax.random.fold_in(own, 1), rows)]
    rotation = jax.random.randint(jax.random.fold_in(own, 2), (rows, 1), 0, top)
    return jnp.take_along_axis(listing, (jnp.arange(top)[None, :] + rotation) % top, axis=1)


def shares(number_of, total, limit, skew, full):
    loads = [(1 << 20) // math.isqrt(standing ** skew) + 1 for standing in range(1, number_of + 1)]
    largest = limit if full else min(limit, max(-(-total // number_of), total * loads[0] // sum(loads)))
    least = 1 if total - largest >= number_of - 1 else 0
    given, spare = [largest] + [least] * (number_of - 1), total - largest - least * (number_of - 1)
    while spare > 0:
        candidates = [i for i in range(1, number_of) if given[i] < largest] or [i for i in range(1, number_of) if given[i] < limit]
        whole, budget = sum([loads[i] for i in candidates]), spare
        for i in candidates:
            extra = min(limit - given[i], max(1, budget * loads[i] // whole), spare)
            given[i] = given[i] + extra
            spare = spare - extra
    return np.array(given)


def centred(rng, extent, deviation, bound, shards=(), held_as=jnp.bfloat16):
    values = deviation * jax.random.normal(rng, extent, jnp.float32)
    if shards:
        values = values * steps_of(rng, extent, shards, -0.22, 0.18)
    return jnp.clip(values, -bound, bound).astype(held_as)


def setup_inputs(seed: int = 0) -> dict:
    splits = jax.random.split(jax.random.key(seed), 24)
    tokens = centred(splits[0], (SEQS, D), 1.0, 6.0, ((0, 128),))
    attn_norm_gain = jnp.clip(1.0 + 0.18 * jax.random.normal(splits[1], (D,), jnp.float32), 0.1, 1.9)
    w_query = centred(splits[2], (D, HEADS * HEAD_DIM), D ** -0.5, 0.125)
    w_key = centred(splits[3], (D, KV_HEADS * HEAD_DIM), D ** -0.5, 0.125)
    w_value = centred(splits[4], (D, KV_HEADS * HEAD_DIM), D ** -0.5, 0.125)
    w_forget = centred(splits[5], (D, HEADS), D ** -0.5, 0.125)
    forget_bias = jnp.clip(jax.random.uniform(splits[6], (HEADS,), jnp.float32, 0.5, 4.0), 0.5, 4.0)
    w_attn_out = centred(splits[7], (HEADS * HEAD_DIM, D), (HEADS * HEAD_DIM) ** -0.5, 0.25)
    cache_keys = draw_cache_keys(jax.random.fold_in(splits[23], 71), 0)
    cache_values = centred(splits[9], (SEQS, CACHE_POSITIONS, KV_HEADS * HEAD_DIM), 1.0, 6.0, ((0, 128),))
    cache_logcum = draw_cache_logcum(jax.random.fold_in(splits[23], 71), 0)
    cache_lengths = with_ends(jax.random.randint(splits[11], (SEQS,), CACHE_POSITIONS // 8, CACHE_POSITIONS + 1), jax.random.fold_in(splits[11], 1), CACHE_POSITIONS // 8, CACHE_POSITIONS).astype(jnp.int32)
    expert_norm_gain = draw_expert_norm_gain(jax.random.fold_in(splits[23], 71), 0)
    expert_ids_keys = jax.random.split(jax.random.fold_in(splits[13], 1), SEQS // SEQ_DEV)
    expert_ids_turns = jax.random.permutation(jax.random.fold_in(splits[13], 3), SEQS // SEQ_DEV)
    expert_ids = jax.vmap(lambda own, number: deal_out(jax.random.fold_in(splits[13], 2), own, number, SEQ_DEV, EXPERTS, TOPK, CAP, 2))(expert_ids_keys, expert_ids_turns).reshape((SEQS, TOPK))
    expert_weights = jnp.clip(jnp.exp(math.log(1.0) - 2.3025851 * jax.random.uniform(splits[14], (SEQS, TOPK), jnp.float32) ** steps_of(splits[14], (SEQS, TOPK), ((0, 128),), -0.2, 0.2)), 0.1, 1.0)
    w_expert_gate = centred(splits[15], (EXPERTS, D, EXPERT_FF), D ** -0.5, 0.125, ((0, 128),))
    w_expert_up = centred(splits[16], (EXPERTS, D, EXPERT_FF), D ** -0.5, 0.125, ((0, 128),))
    w_expert_down = centred(splits[17], (EXPERTS, EXPERT_FF, D), EXPERT_FF ** -0.5, 0.25, ((0, 128),))
    w_dense_gate = centred(splits[18], (D, DENSE_FF), D ** -0.5, 0.125, ((1, 128),))
    w_dense_up = draw_w_dense_up(jax.random.fold_in(splits[23], 71), 0)
    w_dense_down = centred(splits[20], (DENSE_FF, D), DENSE_FF ** -0.5, 0.09375, ((0, 128),))
    dense_norm_gain = jnp.clip(1.0 + 0.18 * jax.random.normal(splits[21], (DENSE_FF,), jnp.float32), 0.1, 1.9)
    branch_gate = centred(splits[22], (D,), D ** -0.5, 0.125, (), jnp.float32)
    return dict(tokens=tokens, attn_norm_gain=attn_norm_gain, w_query=w_query, w_key=w_key, w_value=w_value, w_forget=w_forget, forget_bias=forget_bias, w_attn_out=w_attn_out, cache_keys=cache_keys, cache_values=cache_values, cache_logcum=cache_logcum, cache_lengths=cache_lengths, expert_norm_gain=expert_norm_gain, expert_ids=expert_ids, expert_weights=expert_weights, w_expert_gate=w_expert_gate, w_expert_up=w_expert_up, w_expert_down=w_expert_down, w_dense_gate=w_dense_gate, w_dense_up=w_dense_up, w_dense_down=w_dense_down, dense_norm_gain=dense_norm_gain, branch_gate=branch_gate)


EPS = 1e-06
LIMIT = 7.0
ALPHA = 1.702

def normalize(values, gain):
    return values * lax.rsqrt(lax.optimization_barrier(jnp.mean(values * values, axis=-1, keepdims=True)) + EPS) * gain

def stored(values):
    return lax.optimization_barrier(values.astype(jnp.bfloat16))

def attend(query, key_new, value_new, log_forget, cache_keys, cache_values, cache_logcum, cache_lengths):
    seqs, length = (cache_keys.shape[0], cache_keys.shape[1])
    group = HEADS // KV_HEADS
    scale = HEAD_DIM ** (-0.5)
    heads_q = query.astype(jnp.float32).reshape(seqs, KV_HEADS, group, HEAD_DIM)
    keys = cache_keys.astype(jnp.float32).reshape(seqs, length, KV_HEADS, HEAD_DIM)
    values = cache_values.astype(jnp.float32).reshape(seqs, length, KV_HEADS, HEAD_DIM)
    own_key = key_new.astype(jnp.float32).reshape(seqs, KV_HEADS, HEAD_DIM)
    own_value = value_new.astype(jnp.float32).reshape(seqs, KV_HEADS, 1, HEAD_DIM)
    last_index = jnp.broadcast_to((cache_lengths - 1)[:, None, None], (seqs, HEADS, 1)).astype(jnp.int32)
    carried = jnp.take_along_axis(cache_logcum, last_index, axis=2)[:, :, 0] + log_forget
    offset = (carried[:, :, None] - cache_logcum).reshape(seqs, KV_HEADS, group, length)
    scores = jnp.einsum('skgd,slkd->skgl', heads_q, keys) * scale + offset
    live = jnp.arange(length, dtype=jnp.int32)[None, :] < cache_lengths[:, None]
    scores = jnp.where(live[:, None, None, :], scores, -jnp.inf)
    own = jnp.einsum('skgd,skd->skg', heads_q, own_key) * scale
    top = jnp.maximum(lax.optimization_barrier(jnp.max(scores, axis=-1)), own)
    expo = jnp.exp(scores - top[..., None])
    own_expo = jnp.exp(own - top)
    total = lax.optimization_barrier(jnp.sum(expo, axis=-1)) + own_expo
    weights = stored(expo / total[..., None]).astype(jnp.float32)
    own_weight = stored(own_expo / total).astype(jnp.float32)
    out = jnp.einsum('skgl,slkd->skgd', weights, values) + own_weight[..., None] * own_value
    return out.reshape(seqs, HEADS * HEAD_DIM).astype(jnp.bfloat16)

def expert_unit(rows, gate_w, up_w, down_w):
    gate = jnp.minimum(jnp.dot(rows, gate_w, preferred_element_type=jnp.float32), LIMIT)
    up = jnp.clip(jnp.dot(rows, up_w, preferred_element_type=jnp.float32), -LIMIT, LIMIT)
    act = ((up + 1.0) * gate * jax.nn.sigmoid(gate * ALPHA)).astype(jnp.bfloat16)
    return jnp.dot(act, down_w, preferred_element_type=jnp.float32).astype(jnp.bfloat16)

def reference(tokens, attn_norm_gain, w_query, w_key, w_value, w_forget, forget_bias, w_attn_out, cache_keys, cache_values, cache_logcum, cache_lengths, expert_norm_gain, expert_ids, expert_weights, w_expert_gate, w_expert_up, w_expert_down, w_dense_gate, w_dense_up, w_dense_down, dense_norm_gain, branch_gate):
    seqs = tokens.shape[0]
    normed = normalize(tokens.astype(jnp.float32), attn_norm_gain).astype(jnp.bfloat16)
    query = jnp.dot(normed, w_query, preferred_element_type=jnp.float32).astype(jnp.bfloat16)
    key_new = jnp.dot(normed, w_key, preferred_element_type=jnp.float32).astype(jnp.bfloat16)
    value_new = jnp.dot(normed, w_value, preferred_element_type=jnp.float32).astype(jnp.bfloat16)
    log_forget = jax.nn.log_sigmoid(jnp.dot(normed, w_forget, preferred_element_type=jnp.float32) + forget_bias)

    def one_block(index):
        start = index * SEQ_DEV

        def pick(array):
            return lax.dynamic_slice_in_dim(array, start, SEQ_DEV, 0)
        return attend(pick(query), pick(key_new), pick(value_new), pick(log_forget), pick(cache_keys), pick(cache_values), pick(cache_logcum), pick(cache_lengths))
    attended = lax.map(one_block, jnp.arange(N_EP, dtype=jnp.int32)).reshape(seqs, HEADS * HEAD_DIM)
    mixed = stored(tokens.astype(jnp.float32) + jnp.dot(attended, w_attn_out, preferred_element_type=jnp.float32))
    routed_in = normalize(mixed.astype(jnp.float32), expert_norm_gain).astype(jnp.bfloat16)
    flat_ids = expert_ids.reshape(-1)
    rows_all = flat_ids.shape[0]
    room = N_EP * CAP

    def run_expert(outputs, expert):
        chosen = flat_ids == expert
        order = jnp.cumsum(chosen.astype(jnp.int32)) - 1
        where_to = jnp.where(chosen, order, room).astype(jnp.int32)
        source = jnp.zeros((room,), jnp.int32).at[where_to].set(jnp.arange(rows_all, dtype=jnp.int32), mode='drop')
        picked = jnp.take(routed_in, source // TOPK, axis=0)
        answer = expert_unit(picked, w_expert_gate[expert], w_expert_up[expert], w_expert_down[expert])
        filled = jnp.arange(room, dtype=jnp.int32) < jnp.sum(chosen.astype(jnp.int32))
        target = jnp.where(filled, source, rows_all).astype(jnp.int32)
        return (outputs.at[target].set(answer, mode='drop'), None)
    outputs = lax.scan(run_expert, jnp.zeros((rows_all, D), jnp.bfloat16), jnp.arange(EXPERTS, dtype=jnp.int32))[0]
    routed = lax.optimization_barrier(jnp.sum(expert_weights[:, :, None] * outputs.astype(jnp.float32).reshape(seqs, TOPK, D), axis=1))
    gate_dense = jnp.dot(routed_in, w_dense_gate, preferred_element_type=jnp.float32)
    up_dense = jnp.dot(routed_in, w_dense_up, preferred_element_type=jnp.float32)
    units = stored(jax.nn.silu(gate_dense) * up_dense).astype(jnp.float32)
    unit_scale = lax.rsqrt(lax.optimization_barrier(jnp.mean(units * units, axis=1, keepdims=True)) + EPS)
    hidden = (units * unit_scale * dense_norm_gain).astype(jnp.bfloat16)
    dense = jnp.dot(hidden, w_dense_down, preferred_element_type=jnp.float32)
    branch_scale = jax.nn.sigmoid(lax.optimization_barrier(jnp.sum(routed_in.astype(jnp.float32) * branch_gate, axis=1, keepdims=True)))
    return (mixed.astype(jnp.float32) + routed + branch_scale * dense).astype(jnp.bfloat16)
```

```python
import jax
import jax.numpy as jnp
from jax import lax
from jax.experimental import pallas as pl
from jax.experimental.pallas import tpu as pltpu
from jax.sharding import PartitionSpec as P

MESH = pl.DeviceIdType.MESH
F32 = jnp.float32
BF16 = jnp.bfloat16

N = 128
T = 18
D = 2048
KT = 16
LEN = 1024
HEADS = 8
FF = 512
UNITS = 32
GROUP = 16
GU = 256
EPS = 1e-06
LIMIT = 7.0
ALPHA = 1.702
SEQ_STEP = 6

NT = (((1,), (1,)), ((), ()))


def dot(a, b):
    return jnp.dot(a, b, preferred_element_type=F32)


def dot_nt(a, b):
    return lax.dot_general(a, b, NT, preferred_element_type=F32)


def iota(shape, dim):
    return lax.broadcasted_iota(jnp.int32, shape, dim)


def normalize(values, gain):
    mean = jnp.mean(values * values, axis=-1, keepdims=True)
    return values * lax.rsqrt(mean + EPS) * gain


def onehot(mask):
    return jnp.where(mask, 1.0, 0.0).astype(BF16)


def kernel(
    lens,
    tokens,
    attn_gain,
    wf_t,
    forget_bias,
    expert_gain,
    ids_t,
    ew_t,
    dense_gain,
    branch_gate,
    wq_h,
    wk_h,
    wv_h,
    wo_h,
    ck_h,
    cv_h,
    cl_h,
    weg_h,
    weu_h,
    wed_h,
    wdg_h,
    wdu_h,
    wdd_h,
    out,
    bounce_x,
    bounce_y,
    bounce_r,
    bounce_p,
    wq,
    wk,
    wv,
    wo,
    ck,
    cv,
    cl,
    weg,
    weu,
    wed,
    wgu,
    wdd,
    qs,
    os,
    mixed,
    xs,
    xr,
    ys,
    yr,
    rk,
    rp,
    ps,
    rr,
    ssv,
    ssr,
    w_sem,
    kv_sem,
    own_sem,
    gs_sem,
    gr_sem,
    fs_sem,
    fr_sem,
    a_sem,
):
    me = lax.axis_index("ep")
    z = me // 32
    p = lax.rem(me, 32)
    q = p // 2
    c = lax.rem(p, 2)
    block = z * 2 + c

    barrier = pltpu.get_barrier_semaphore()

    def greet(i, carry):
        pl.semaphore_signal(
            barrier, inc=1, device_id=(lax.rem(me + i, N),), device_id_type=MESH
        )
        return carry

    lax.fori_loop(1, N, greet, 0)

    def fetch(src, dst, sem):
        return pltpu.make_async_copy(src, dst, sem)

    first = [
        fetch(wq_h, wq, w_sem.at[0]),
        fetch(wk_h, wk, w_sem.at[1]),
        fetch(wv_h, wv, w_sem.at[2]),
    ]
    for copy in first:
        copy.start()

    def caches(s):
        return (
            fetch(ck_h.at[s], ck.at[s], kv_sem.at[0, s]),
            fetch(cl_h.at[s], cl.at[s], kv_sem.at[1, s]),
            fetch(cv_h.at[s], cv.at[s], kv_sem.at[2, s]),
        )

    def start_cache(s, carry):
        for copy in caches(s):
            copy.start()
        return carry

    lax.fori_loop(0, T, start_cache, 0)
    rows_b = pl.ds(pl.multiple_of(block * UNITS, UNITS), UNITS)
    rows_u = pl.ds(pl.multiple_of(GU + block * UNITS, UNITS), UNITS)
    late = [
        fetch(wo_h, wo, w_sem.at[3]),
        fetch(wdg_h, wgu.at[rows_b], w_sem.at[4]),
        fetch(wdu_h, wgu.at[rows_u], w_sem.at[5]),
        fetch(wdd_h, wdd.at[rows_b], w_sem.at[6]),
        fetch(weg_h.at[0], weg, w_sem.at[7]),
        fetch(weu_h.at[0], weu, w_sem.at[8]),
        fetch(wed_h.at[0], wed, w_sem.at[9]),
    ]
    for copy in late:
        copy.start()

    expert = iota((N, T), 0)
    member = jnp.zeros((N, T), F32)
    weight = jnp.zeros((N, T), F32)
    for k in range(6):
        named = ids_t[k : k + 1, :] == expert
        member = jnp.where(named, 1.0, member)
        weight = jnp.where(named, ew_t[k : k + 1, :], weight)
    upper = onehot(iota((T, T), 0) <= iota((T, T), 1))
    order = dot(member.astype(BF16), upper)
    rank = [
        jnp.where((order == r + 1.0) & (member > 0.5), 1.0, 0.0) for r in range(2)
    ]
    spread = [onehot(iota((2 * N, N), 0) == 2 * iota((2 * N, N), 1) + r) for r in range(2)]
    place = sum(dot(spread[r], rank[r].astype(BF16)) for r in range(2)).astype(BF16)
    eye = onehot(iota((24, T), 0) == iota((24, T), 1))
    parts = []
    rest = weight
    for _ in range(3):
        part = rest.astype(BF16)
        rest = rest - part.astype(F32)
        laid = sum(
            dot(spread[r], (part.astype(F32) * rank[r]).astype(BF16)) for r in range(2)
        )
        parts.append(dot_nt(eye, laid.astype(BF16)).astype(BF16))
    combine = jnp.concatenate(parts, axis=0)

    tok = tokens[...].astype(F32)
    normed = normalize(tok, attn_gain[...]).astype(BF16)
    for copy in first:
        copy.wait()
    query = dot(normed, wq[...]).astype(BF16).astype(F32)
    key_new = dot(normed, wk[...]).astype(BF16).astype(F32)
    value_new = dot(normed, wv[...]).astype(BF16).astype(F32)
    bias = jnp.sum(
        jnp.where(iota((8, 8), 0) == iota((8, 8), 1), forget_bias[...], 0.0),
        axis=1,
        keepdims=True,
    )
    raw = dot_nt(wf_t[...], normed) + bias
    log_forget = jnp.minimum(raw, 0.0) - jnp.log1p(jnp.exp(-jnp.abs(raw)))
    low = iota((T, 128), 1) < 64
    for h in range(HEADS):
        tile = query[:, (h // 2) * 128 : (h // 2 + 1) * 128]
        if (h % 2) != (h // 4):
            tile = pltpu.roll(tile, 64, 1)
        qs[:, h, :] = jnp.where(low if h < 4 else ~low, tile, 0.0)
    key_mask = iota((T, 128), 0)
    head_lane = iota((8, T), 1)
    position = iota((8, LEN), 1)

    def sequence(s):
        for copy in caches(s):
            copy.wait()
        qb = qs[s]
        k_row = jnp.sum(jnp.where(key_mask == s, key_new, 0.0), axis=0, keepdims=True)
        v_row = jnp.sum(jnp.where(key_mask == s, value_new, 0.0), axis=0, keepdims=True)
        own = jnp.sum(qb * k_row, axis=1, keepdims=True) * 0.125
        forget = jnp.sum(jnp.where(head_lane == s, log_forget, 0.0), axis=1, keepdims=True)
        logcum = cl[s]
        length = lens[s]
        last = jnp.sum(
            jnp.where(position == length - 1, logcum, 0.0), axis=1, keepdims=True
        )
        carried = last + forget
        scores = dot_nt(qb.astype(BF16), ck[s]) * 0.125 + (carried - logcum)
        scores = jnp.where(position < length, scores, -jnp.inf)
        top = jnp.maximum(jnp.max(scores, axis=1, keepdims=True), own)
        expo = jnp.exp(scores - top)
        own_expo = jnp.exp(own - top)
        scale = 1.0 / (jnp.sum(expo, axis=1, keepdims=True) + own_expo)
        weights = (expo * scale).astype(BF16)
        own_weight = (own_expo * scale).astype(BF16).astype(F32)
        os[s] = dot(weights, cv[s]) + own_weight * v_row

    def sequences(g, carry):
        for i in range(SEQ_STEP):
            sequence(g * SEQ_STEP + i)
        return carry

    sequences(0, 0)

    pl.semaphore_wait(barrier, N - 1)
    for copy in late[1:4]:
        copy.wait()

    def dense_weights(rows, rows_up, i, peer):
        return [
            pltpu.make_async_remote_copy(
                src_ref=ref.at[r],
                dst_ref=ref.at[r],
                send_sem=gs_sem.at[i, j],
                recv_sem=gr_sem.at[i, j],
                device_id=(peer,),
                device_id_type=MESH,
            )
            for j, (ref, r) in enumerate(((wgu, rows), (wgu, rows_up), (wdd, rows)))
        ]

    def block_rows(b):
        return (
            pl.ds(pl.multiple_of(b * UNITS, UNITS), UNITS),
            pl.ds(pl.multiple_of(GU + b * UNITS, UNITS), UNITS),
        )

    for i in range(1, 4):
        for copy in dense_weights(rows_b, rows_u, i, lax.rem(me + 32 * i, N)):
            copy.start()
    partner = me + 1 - 2 * c
    for copy in dense_weights(rows_b, rows_u, 4, partner):
        copy.start()

    lax.fori_loop(1, T // SEQ_STEP, sequences, 0)

    late[0].wait()
    tiles = []
    for t in range(4):
        even, odd = os[:, 2 * t, :], os[:, 2 * t + 1, :]
        if t < 2:
            odd = pltpu.roll(odd, 64, 1)
        else:
            even = pltpu.roll(even, 64, 1)
        tiles.append(jnp.where(low, even, odd))
    attended = jnp.concatenate(tiles, axis=1).astype(BF16)
    mixed[...] = (tok + dot(attended, wo[...])).astype(BF16)
    routed_in = normalize(mixed[...].astype(F32), expert_gain[...]).astype(BF16)
    branch = jax.nn.sigmoid(
        jnp.sum(routed_in.astype(F32) * branch_gate[...], axis=1, keepdims=True)
    )

    for k in range(KT):
        rk[k] = routed_in[:, k * 128 : (k + 1) * 128]
    for n in range(4):
        cols = slice(n * 512, (n + 1) * 512)
        sent = dot(place, routed_in[:, cols]).astype(BF16)
        for k in range(4):
            xs[n * 4 + k] = sent[:, k * 128 : (k + 1) * 128]

    def pair(ref, d):
        return ref.at[:, pl.ds(2 * d, 2), :]

    def exchange(src, dst, i):
        def body(j, carry):
            d = lax.rem(me + j, N)
            pltpu.make_async_remote_copy(
                src_ref=pair(src, d),
                dst_ref=pair(dst, me),
                send_sem=fs_sem.at[i],
                recv_sem=fr_sem.at[i],
                device_id=(d,),
                device_id_type=MESH,
            ).start()
            return carry

        lax.fori_loop(1, N, body, 0)

    def exchanged(src, dst, i):
        return pltpu.make_async_remote_copy(
            src_ref=src.at[:, pl.ds(0, 2 * (N - 1)), :],
            dst_ref=dst.at[:, pl.ds(0, 2 * (N - 1)), :],
            send_sem=fs_sem.at[i],
            recv_sem=fr_sem.at[i],
            device_id=(lax.rem(me + 1, N),),
            device_id_type=MESH,
        )

    def triple(ref, b):
        return ref.at[:, pl.ds(T * b, T), :]

    def mate(i):
        return z * 32 + lax.rem(q + i, GROUP) * 2 + c

    def group_wait(ref, i):
        part = ref.at[:, pl.ds(0, T * (GROUP - 1)), :]
        return pltpu.make_async_remote_copy(
            src_ref=part,
            dst_ref=part,
            send_sem=fs_sem.at[i],
            recv_sem=fr_sem.at[i],
            device_id=(mate(1),),
            device_id_type=MESH,
        )

    exchange(xs, xr, 0)
    own_x = fetch(pair(xs, me), bounce_x, own_sem.at[0])
    own_r = fetch(rk, bounce_r, own_sem.at[1])
    own_x.start()
    own_r.start()
    for i in range(1, GROUP):
        pltpu.make_async_remote_copy(
            src_ref=rk,
            dst_ref=triple(rp, q),
            send_sem=fs_sem.at[2],
            recv_sem=fr_sem.at[2],
            device_id=(mate(i),),
            device_id_type=MESH,
        ).start()
    own_x.wait()
    own_r.wait()
    own_x = fetch(bounce_x, pair(xr, me), own_sem.at[0])
    own_r = fetch(bounce_r, triple(rp, q), own_sem.at[1])
    own_x.start()
    own_r.start()

    for i in range(1, 4):
        theirs = block_rows(lax.rem(z + 4 - i, 4) * 2 + c)
        for copy in dense_weights(*theirs, i, partner):
            copy.wait_recv()
        for copy in dense_weights(*theirs, 4 + i, partner):
            copy.start()

    for copy in late[4:]:
        copy.wait()
    own_x.wait()
    exchanged(xs, xr, 0).wait_recv()
    for m in range(2):
        rows = slice(m * 128, (m + 1) * 128)
        x = jnp.concatenate([xr[k, rows, :] for k in range(KT)], axis=1)
        gate = jnp.minimum(dot(x, weg[...]), LIMIT)
        up = jnp.clip(dot(x, weu[...]), -LIMIT, LIMIT)
        act = ((up + 1.0) * gate * jax.nn.sigmoid(gate * ALPHA)).astype(BF16)
        for n in range(4):
            answer = dot(act, wed[:, n * 512 : (n + 1) * 512]).astype(BF16)
            for k in range(4):
                ys[n * 4 + k, rows, :] = answer[:, k * 128 : (k + 1) * 128]
    exchange(ys, yr, 1)
    own_y = fetch(pair(ys, me), bounce_y, own_sem.at[0])
    own_y.start()
    own_y.wait()
    own_y = fetch(bounce_y, pair(yr, me), own_sem.at[0])
    own_y.start()

    lane = iota((1, 128), 1)
    gains = []
    for j in range(4):
        row = dense_gain[pl.ds(j * 8 + q // 2, 1), :]
        odd = jnp.full((1, 128), lax.rem(q, 2), jnp.int32) == 1
        gains.append(jnp.where(odd, pltpu.roll(row, 64, 1), row))
    gain = jnp.concatenate(
        [
            jnp.where(lane < 64, gains[2 * j], pltpu.roll(gains[2 * j + 1], 64, 1))
            for j in range(2)
        ],
        axis=1,
    )
    for copy in dense_weights(*block_rows(z * 2 + 1 - c), 4, partner):
        copy.wait_recv()
    for i in range(1, 4):
        theirs = block_rows(lax.rem(z + 4 - i, 4) * 2 + 1 - c)
        for copy in dense_weights(*theirs, 4 + i, partner):
            copy.wait_recv()
    own_r.wait()
    group_wait(rp, 2).wait_recv()
    ones = jnp.ones((8, GU), BF16)
    ssv[...] = jnp.zeros_like(ssv)
    for m in range(3):
        rows = slice(m * 96, (m + 1) * 96)
        r = jnp.concatenate([rp[k, rows, :] for k in range(KT)], axis=1)
        both = dot_nt(r, wgu[...])
        gate, up = both[:, :GU], both[:, GU:]
        units = (gate * jax.nn.sigmoid(gate) * up).astype(BF16).astype(F32)
        square = units * units
        high = square.astype(BF16)
        rest = (square - high.astype(F32)).astype(BF16)
        total = dot_nt(ones, high) + dot_nt(ones, rest)
        ssv[:, m * 128 : m * 128 + 96] = total[0:1, :]
        hidden = (units * gain).astype(BF16)
        for n in range(4):
            part = dot(hidden, wdd[:, n * 512 : (n + 1) * 512]).astype(BF16)
            for k in range(4):
                ps[n * 4 + k, rows, :] = part[:, k * 128 : (k + 1) * 128]

    def sums(i):
        return pltpu.make_async_remote_copy(
            src_ref=ssv,
            dst_ref=ssr.at[q],
            send_sem=fs_sem.at[4],
            recv_sem=fr_sem.at[4],
            device_id=(mate(i),),
            device_id_type=MESH,
        )

    for i in range(1, GROUP):
        other = lax.rem(q + i, GROUP)
        pltpu.make_async_remote_copy(
            src_ref=triple(ps, other),
            dst_ref=triple(rr, q),
            send_sem=fs_sem.at[3],
            recv_sem=fr_sem.at[3],
            device_id=(mate(i),),
            device_id_type=MESH,
        ).start()
        sums(i).start()
    own_p = fetch(triple(ps, q), bounce_p, own_sem.at[1])
    own_p.start()
    ssr[q] = ssv[...]
    own_p.wait()
    own_p = fetch(bounce_p, triple(rr, q), own_sem.at[1])
    own_p.start()

    own_y.wait()
    exchanged(ys, yr, 1).wait_recv()
    own_p.wait()
    group_wait(rr, 3).wait_recv()
    some = ssr.at[pl.ds(0, GROUP - 1)]
    sum_wait = pltpu.make_async_remote_copy(
        src_ref=some,
        dst_ref=some,
        send_sem=fs_sem.at[4],
        recv_sem=fr_sem.at[4],
        device_id=(mate(1),),
        device_id_type=MESH,
    )
    sum_wait.wait_recv()
    total = ssr[0]
    for i in range(1, GROUP):
        total = total + ssr[i]
    spot = T * q + iota((T, 384), 0)
    spot = spot + (spot // 96) * 32
    squares = jnp.sum(
        jnp.where(iota((T, 384), 1) == spot, total, 0.0), axis=1, keepdims=True
    )
    scale = branch * lax.rsqrt(squares * (1.0 / 4096.0) + EPS)
    gather = onehot(lax.rem(iota((T, T * GROUP), 1), T) == iota((T, T * GROUP), 0))
    for n in range(4):
        y = jnp.concatenate([yr[n * 4 + k] for k in range(4)], axis=1)
        three = dot(combine, y)
        routed = three[0:24] + three[24:48] + three[48:72]
        r = jnp.concatenate([rr[n * 4 + k] for k in range(4)], axis=1)
        dense = dot(gather, r)
        cols = slice(n * 512, (n + 1) * 512)
        out[:, cols] = (
            mixed[:, cols].astype(F32) + routed[0:T] + scale * dense
        ).astype(BF16)

    exchanged(xs, xr, 0).wait_send()
    exchanged(ys, yr, 1).wait_send()
    group_wait(rp, 2).wait_send()
    group_wait(rr, 3).wait_send()
    sum_wait.wait_send()
    for i in range(1, 8):
        for copy in dense_weights(rows_b, rows_u, i, partner):
            copy.wait_send()


def shards(
    tokens,
    attn_norm_gain,
    w_query,
    w_key,
    w_value,
    w_forget,
    forget_bias,
    w_attn_out,
    cache_keys,
    cache_values,
    cache_logcum,
    cache_lengths,
    expert_norm_gain,
    expert_ids,
    expert_weights,
    w_expert_gate,
    w_expert_up,
    w_expert_down,
    w_dense_gate,
    w_dense_up,
    w_dense_down,
    dense_norm_gain,
    branch_gate,
):
    vmem = pl.BlockSpec(memory_space=pltpu.VMEM)
    hbm = pl.BlockSpec(memory_space=pl.ANY)
    dma = pltpu.SemaphoreType.DMA
    result = pl.pallas_call(
        kernel,
        out_shape=(
            jax.ShapeDtypeStruct((T, D), BF16),
            jax.ShapeDtypeStruct((KT, 2, 128), BF16),
            jax.ShapeDtypeStruct((KT, 2, 128), BF16),
            jax.ShapeDtypeStruct((KT, T, 128), BF16),
            jax.ShapeDtypeStruct((KT, T, 128), BF16),
        ),
        in_specs=[pl.BlockSpec(memory_space=pltpu.SMEM)] + [vmem] * 9 + [hbm] * 13,
        out_specs=(vmem, hbm, hbm, hbm, hbm),
        scratch_shapes=[
            pltpu.VMEM((D, 512), BF16),
            pltpu.VMEM((D, 128), BF16),
            pltpu.VMEM((D, 128), BF16),
            pltpu.VMEM((512, D), BF16),
            pltpu.VMEM((T, LEN, 128), BF16),
            pltpu.VMEM((T, LEN, 128), BF16),
            pltpu.VMEM((T, HEADS, LEN), F32),
            pltpu.VMEM((D, FF), BF16),
            pltpu.VMEM((D, FF), BF16),
            pltpu.VMEM((FF, D), BF16),
            pltpu.VMEM((2 * GU, D), BF16),
            pltpu.VMEM((GU, D), BF16),
            pltpu.VMEM((T, HEADS, 128), F32),
            pltpu.VMEM((T, HEADS, 128), F32),
            pltpu.VMEM((T, D), BF16),
            pltpu.VMEM((KT, 2 * N, 128), BF16),
            pltpu.VMEM((KT, 2 * N, 128), BF16),
            pltpu.VMEM((KT, 2 * N, 128), BF16),
            pltpu.VMEM((KT, 2 * N, 128), BF16),
            pltpu.VMEM((KT, T, 128), BF16),
            pltpu.VMEM((KT, T * GROUP, 128), BF16),
            pltpu.VMEM((KT, T * GROUP, 128), BF16),
            pltpu.VMEM((KT, T * GROUP, 128), BF16),
            pltpu.VMEM((1, 384), F32),
            pltpu.VMEM((GROUP, 1, 384), F32),
            dma((10,)),
            dma((3, T)),
            dma((2,)),
            dma((8, 3)),
            dma((8, 3)),
            dma((5,)),
            dma((5,)),
            dma((1,)),
        ],
        compiler_params=pltpu.CompilerParams(
            collective_id=0, has_side_effects=True, vmem_limit_bytes=60 << 20
        ),
    )(
        cache_lengths,
        tokens,
        attn_norm_gain.reshape(1, D),
        w_forget.T,
        forget_bias.reshape(1, HEADS),
        expert_norm_gain.reshape(1, D),
        expert_ids.T,
        expert_weights.T,
        dense_norm_gain.reshape(32, 128),
        branch_gate.reshape(1, D),
        w_query,
        w_key,
        w_value,
        w_attn_out,
        cache_keys,
        cache_values,
        cache_logcum,
        w_expert_gate,
        w_expert_up,
        w_expert_down,
        w_dense_gate.T,
        w_dense_up.T,
        w_dense_down,
    )
    return result[0]


def solution(mesh):
    in_specs = (
        P("ep", None),
        P(),
        P(),
        P(),
        P(),
        P(),
        P(),
        P(),
        P("ep", None, None),
        P("ep", None, None),
        P("ep", None, None),
        P("ep"),
        P(),
        P("ep", None),
        P("ep", None),
        P("ep", None, None),
        P("ep", None, None),
        P("ep", None, None),
        P(None, "ep"),
        P(None, "ep"),
        P("ep", None),
        P(),
        P(),
    )
    out_specs = P("ep", None)
    return jax.shard_map(shards, mesh=mesh, in_specs=in_specs, out_specs=out_specs, check_vma=False)
```
